32 devices in a mesh: sp: 4 (over y, core), dp: 8 (over z, x).
Axes of the slice: x: 2, y: 2, z: 4, core: 2. Of those that a mesh axis runs over, the one named last changes fastest.
Arguments:
- queries: bfloat16 [8, 704, 2048], P('dp', 'sp'), may hold values from -24 to 24, as said below
- keys: bfloat16 [8, 704, 256], P('dp', 'sp'), may hold values from -24 to 24, as said below
- tokens: bfloat16 [8, 704, 2304], P('dp', 'sp'), may hold values from -18 to 18
- w_value: bfloat16 [2304, 256], P('dp'), may hold values from -0.125 to 0.125
- q_gain: float32 [128], replicated, may hold values from 0.5 to 6, as said below
- k_gain: float32 [128], replicated, may hold values from 0.5 to 6, as said below
Outputs:
- attended: bfloat16 [8, 704, 2048], P('dp', 'sp')
The draws below stay inside these ranges and needn't reach their ends.
Inputs may be any that keep to these rules, and one draw needn't show every extreme that they name: `queries`: real-valued projected query entries. `keys`: real-valued projected key entries. `q_gain`: positive gains. `k_gain`: positive gains.
All inputs are finite; a program needn't handle non-finite values.
Results may differ from the reference program's by a relative error of at most 0.0022.
The reference program's roundings to bfloat16 on the way (of `values`, `query_rot`, `key_rot` and `probability`) count: a program that leaves them out, or rounds other values in their place, can miss the bound.
Values may be sent and summed in bfloat16 or wider, within the bound.
A program may use at most 64 MiB of HBM per device.

```python
import math
import jax
import jax.numpy as jnp
from jax import lax

D = 2304
HD = 128
QH = 16
KVH = 2
GRID_W = 64
LEN = 704
BATCH = 8


def shared_pair(key):
    key_draw = jnp.clip(jax.random.normal(jax.random.fold_in(key, 11), (BATCH, LEN, KVH * HD), jnp.float32), -6.0, 6.0)
    query_draw = jnp.clip(jax.random.normal(jax.random.fold_in(key, 12), (BATCH, LEN, QH * HD), jnp.float32), -6.0, 6.0)
    return (query_draw, key_draw)


def draw_queries(key, part):
    return shared_pair(key)[0].astype(jnp.bfloat16)


def draw_keys(key, part):
    return shared_pair(key)[1].astype(jnp.bfloat16)


def gain_draw(key):
    return jnp.exp(jax.random.uniform(key, (HD,), jnp.float32, jnp.log(0.6), jnp.log(1.8)))


def draw_q_gain(key, part):
    return gain_draw(jax.random.fold_in(key, 21))


def draw_k_gain(key, part):
    return gain_draw(jax.random.fold_in(key, 22))


def levels(stream_key, dims, shards, smallest, top_value):
    def one(dim, parts):
        heights = jax.random.uniform(jax.random.fold_in(jax.random.fold_in(stream_key, 6), dim), (parts,), jnp.float32, smallest / len(shards), top_value / len(shards))
        return jnp.repeat(jnp.exp(heights), dims[dim] // parts).reshape((-1,) + (1,) * (len(dims) - dim - 1))

    level = one(*shards[0])
    for cut in shards[1:]:
        level = level * one(*cut)
    return level


def normal_values(stream_key, shape, width, most, shards=(), kind=jnp.bfloat16):
    array = jax.random.normal(stream_key, shape, jnp.float32) * width
    if len(shards) > 0:
        array = levels(stream_key, shape, shards, -0.22, 0.18) * array
    return jnp.clip(array, min=-most, max=most).astype(kind)


def setup_inputs(seed: int = 0) -> dict:
    key_list = jax.random.split(jax.random.key(seed), 7)
    queries = draw_queries(jax.random.fold_in(key_list[6], 71), 0)
    keys = draw_keys(jax.random.fold_in(key_list[6], 71), 0)
    tokens = normal_values(key_list[2], (BATCH, LEN, D), 3.0, 18.0, ((0, 8), (1, 4)))
    w_value = normal_values(key_list[3], (D, KVH * HD), D ** -0.5, 0.125, ((0, 8),))
    q_gain = draw_q_gain(jax.random.fold_in(key_list[6], 71), 0)
    k_gain = draw_k_gain(jax.random.fold_in(key_list[6], 71), 0)
    return {"queries": queries, "keys": keys, "tokens": tokens, "w_value": w_value, "q_gain": q_gain, "k_gain": k_gain}


epsilon = 1e-06

def unit_rms(vectors, scaling):
    return vectors * lax.rsqrt(lax.optimization_barrier(jnp.mean(vectors * vectors, axis=-1, keepdims=True)) + epsilon) * scaling

def rotary(vectors, row_pos, col_pos):
    head_width = vectors.shape[-1]
    half_width = head_width // 2
    quarter = half_width // 2
    frequency = 10000.0 ** (-jnp.arange(quarter, dtype=jnp.float32) * 2.0 / half_width)

    def rotate_half(section, angle_pos):
        angles = angle_pos[:, None, None] * frequency
        cosine = jnp.cos(angles)
        sine_table = jnp.sin(angles)
        leading = section[..., :quarter]
        second = section[..., quarter:]
        return jnp.concatenate([leading * cosine - second * sine_table, second * cosine + leading * sine_table], axis=-1)
    return jnp.concatenate([rotate_half(vectors[..., :half_width], row_pos), rotate_half(vectors[..., half_width:], col_pos)], axis=-1)

def reference(queries, keys, tokens, w_value, q_gain, k_gain):
    group = QH // KVH
    positions = jnp.arange(LEN, dtype=jnp.int32)
    row_pos = (positions // GRID_W).astype(jnp.float32)
    col_pos = (positions % GRID_W).astype(jnp.float32)
    block_rows = math.gcd(LEN, 512)

    def one_sequence(inputs):
        query_rows, key_rows, token_rows = inputs
        values = jnp.dot(token_rows, w_value, preferred_element_type=jnp.float32)
        values = lax.optimization_barrier(values.astype(jnp.bfloat16)).astype(jnp.float32).reshape(LEN, KVH, HD)
        query_norm = unit_rms(query_rows.astype(jnp.float32).reshape(LEN, QH, HD), q_gain.astype(jnp.float32))
        query_rot = lax.optimization_barrier(rotary(query_norm, row_pos, col_pos).astype(jnp.bfloat16)).astype(jnp.float32)
        key_norm = unit_rms(key_rows.astype(jnp.float32).reshape(LEN, KVH, HD), k_gain.astype(jnp.float32))
        key_rot = lax.optimization_barrier(rotary(key_norm, row_pos, col_pos).astype(jnp.bfloat16)).astype(jnp.float32)
        blocked = query_rot.reshape(LEN // block_rows, block_rows, KVH, group, HD)

        def one_block(query_block):
            scores = jnp.einsum('qkgd,nkd->kgqn', query_block, key_rot) * HD ** (-0.5)
            highest = lax.optimization_barrier(jnp.max(scores, axis=-1, keepdims=True))
            weights = jnp.exp(scores - highest)
            weights = weights / lax.optimization_barrier(jnp.sum(weights, axis=-1, keepdims=True))
            probability = lax.optimization_barrier(weights.astype(jnp.bfloat16)).astype(jnp.float32)
            blended = jnp.einsum('kgqn,nkd->qkgd', probability, values)
            return blended.astype(jnp.bfloat16).reshape(block_rows, QH * HD)
        return lax.map(one_block, blocked).reshape(LEN, QH * HD)
    return lax.map(one_sequence, (queries, keys, tokens))
```

```python
import functools
import math

import jax
import jax.numpy as jnp
from jax import lax
from jax.experimental import pallas as pl
from jax.experimental.pallas import tpu as pltpu
from jax.sharding import PartitionSpec as P

HD = 128
QH = 16
KVH = 2
GRID_W = 64
GROUP = QH // KVH
epsilon = 1e-06
MESH = pl.DeviceIdType.MESH


def inner_size(n):
    size = 1
    while size * size * 4 <= n and n % (size * 2) == 0:
        size *= 2
    return size


def partner(index, d, n):
    if n & (n - 1):
        return (index + d) % n
    bit = 1
    while bit <= d:
        if d & bit:
            index = index + bit - 2 * bit * (index // bit % 2)
        bit *= 2
    return index


def kernel(
    n_sp, n_dp, q_hbm, k_hbm, tok_hbm, w_hbm, qg_hbm, kg_hbm, out_ref,
    q_in, k_in, tok, wbuf, kbuf, vbuf, qrot, prob, cos_ref, sin_ref, cosg_ref, sing_ref, perm_ref, qg_ref, kg_ref,
    in_sem, w_z, w_x, w_d, w_recv, t_send, t_recv, k_send, k_recv, k_fwd, k_frecv, v_send, v_recv, v_fwd, v_frecv,
):
    rows = q_hbm.shape[0]
    depth = w_hbm.shape[0]
    length = kbuf.shape[0]
    n_x = inner_size(n_dp)
    n_z = n_dp // n_x
    n_y = n_sp // 2
    sp = lax.axis_index("sp")
    dp = lax.axis_index("dp")
    z, x = dp // n_x, dp % n_x
    y, c = sp // 2, sp % 2
    sib = y * 2 + (1 - c)

    def block(d):
        return wbuf.at[pl.ds(pl.multiple_of(d * depth, 16), depth), :]

    def token_part(core):
        return tok.at[pl.ds(pl.multiple_of(core * rows, 16), rows), :]

    z_peers = [partner(z, d, n_z) for d in range(1, n_z)]
    x_peers = [((x + d) % n_x) for d in range(1, n_x)]
    y_peers = [((y + d) % n_y) for d in range(1, n_y)]
    back = 0 if n_z & (n_z - 1) == 0 else n_z - 2
    diagonal = sorted({0, back}) if n_z > 1 else []

    with jax.named_scope("signal"):
        barrier = pltpu.get_barrier_semaphore()
        for zp in z_peers:
            pl.semaphore_signal(barrier, inc=1, device_id=(sp, zp * n_x + x), device_id_type=MESH)
        for xp in x_peers:
            pl.semaphore_signal(barrier, inc=1, device_id=(sp, z * n_x + xp), device_id_type=MESH)
            for i in diagonal:
                pl.semaphore_signal(barrier, inc=1, device_id=(sp, z_peers[i] * n_x + xp), device_id_type=MESH)
        for yp in y_peers:
            pl.semaphore_signal(barrier, inc=1, device_id=(yp * 2 + c, dp), device_id_type=MESH)
        pl.semaphore_signal(barrier, inc=1, device_id=(sib, dp), device_id_type=MESH)

        w_mine = w_hbm.at[:, pl.ds(pl.multiple_of(c * HD, HD), HD)]
        loads = [
            pltpu.make_async_copy(src, dst, in_sem.at[i])
            for i, (src, dst) in enumerate(
                (
                    (w_mine, block(dp)), (k_hbm, k_in), (kg_hbm, kg_ref), (tok_hbm, token_part(c)),
                    (q_hbm, q_in), (qg_hbm, qg_ref),
                )
            )
        ]
        for load in loads:
            load.start()

    pending = []

    def remote(src, dst, send, recv, where):
        return pltpu.make_async_remote_copy(
            src_ref=src, dst_ref=dst, send_sem=send, recv_sem=recv, device_id=where, device_id_type=MESH
        )

    def send(*args):
        copy = remote(*args)
        copy.start()
        pending.append(copy)

    with jax.named_scope("w_send"):
        loads[0].wait()
        pl.semaphore_wait(barrier, n_z - 1 + (n_x - 1) * (1 + len(diagonal)) + n_y)
        for k, xp in enumerate(x_peers):
            send(block(dp), block(dp), w_x.at[0, k], w_recv.at[dp], (sp, z * n_x + xp))
        for i, zp in enumerate(z_peers):
            send(block(dp), block(dp), w_z.at[i], w_recv.at[dp], (sp, zp * n_x + x))
        if n_z > 1:
            for k, xp in enumerate(x_peers):
                send(block(dp), block(dp), w_d.at[k], w_recv.at[dp], (sp, z_peers[0] * n_x + xp))

    with jax.named_scope("tables"):
        pos = sp * rows + lax.broadcasted_iota(jnp.int32, (rows, HD), 0)
        lane = lax.broadcasted_iota(jnp.int32, (rows, HD), 1)
        grid_row = pos // GRID_W
        coord = jnp.where(lane < HD // 2, grid_row, pos - grid_row * GRID_W).astype(jnp.float32)
        step = (lax.broadcasted_iota(jnp.int32, (1, HD), 1) % (HD // 4)).astype(jnp.float32)
        angles = coord * jnp.exp2(step * (-2.0 * math.log2(10000.0) / (HD // 2)))
        cos_ref[...] = jnp.cos(angles)
        sine = jnp.sin(angles)
        sin_ref[...] = jnp.where(lane % (HD // 2) < HD // 4, -sine, sine)
        source = lax.broadcasted_iota(jnp.int32, perm_ref.shape, 0)
        target = lax.broadcasted_iota(jnp.int32, perm_ref.shape, 1)
        swapped = jnp.where(target % (HD // 2) < HD // 4, target + HD // 4, target - HD // 4)
        perm_ref[...] = (source == swapped).astype(jnp.float32).astype(jnp.bfloat16)

    def gained(gain_ref):
        gain = gain_ref[...]
        wide = jnp.broadcast_to(gain, (8, HD))
        lanes = lax.broadcasted_iota(jnp.int32, (8, HD), 1)
        other = jnp.where(
            lanes % (HD // 2) < HD // 4, pltpu.roll(wide, HD - HD // 4, 1), pltpu.roll(wide, HD // 4, 1)
        )[:1]
        cosg_ref[...] = cos_ref[...] * gain
        sing_ref[...] = sin_ref[...] * other

    def norm_rot(pair):
        other = jnp.dot(pair, perm_ref[...], preferred_element_type=jnp.float32)
        heads = []
        for j in range(2):
            u = pair[:, j * HD:(j + 1) * HD].astype(jnp.float32)
            inverse = lax.rsqrt(jnp.mean(u * u, axis=-1, keepdims=True) + epsilon)
            turned = u * cosg_ref[...] + other[:, j * HD:(j + 1) * HD] * sing_ref[...]
            heads.append((turned * inverse).astype(jnp.bfloat16))
        return heads

    def at(ref, s):
        return ref.at[pl.ds(pl.multiple_of(s * rows, 16), rows), :]

    own = pl.ds(pl.multiple_of(sp * rows, 16), rows)
    with jax.named_scope("k_norm"):
        loads[1].wait()
        loads[2].wait()
        gained(kg_ref)
        for g, head in enumerate(norm_rot(k_in[...])):
            kbuf[own, g * HD:(g + 1) * HD] = head

    with jax.named_scope("k_send"):
        for i, yp in enumerate(y_peers):
            send(at(kbuf, sp), at(kbuf, sp), k_send.at[i], k_recv.at[y], (yp * 2 + c, dp))
        send(at(kbuf, sp), at(kbuf, sp), k_send.at[n_y - 1], k_frecv.at[y], (sib, dp))
        loads[3].wait()
        send(token_part(c), token_part(c), t_send.at[0], t_recv.at[0], (sib, dp))

    with jax.named_scope("q_norm"):
        loads[4].wait()
        loads[5].wait()
        gained(qg_ref)
        for b in range(QH // 2):
            for j, head in enumerate(norm_rot(q_in[:, 2 * b * HD:(2 * b + 2) * HD])):
                g, i = divmod(2 * b + j, GROUP)
                qrot[g, i * rows:(i + 1) * rows] = head

    def arrived(d):
        remote(block(d), block(d), w_z.at[0], w_recv.at[d], (sp, d)).wait_recv()

    def relay(i):
        d = z_peers[i] * n_x + x
        arrived(d)
        if i != back:
            for k, xp in enumerate(x_peers):
                send(block(d), block(d), w_x.at[i + 1, k], w_recv.at[d], (sp, z * n_x + xp))

    order = [i for i in range(n_z - 1) if i != back]
    order = order[::-1]
    scale = HD ** -0.5 * math.log2(math.e)

    def weights(g, start, size):
        s = lax.dot_general(
            kbuf[:, g * HD:(g + 1) * HD], qrot[g, start:start + size], (((1,), (1,)), ((), ())),
            preferred_element_type=jnp.float32,
        )
        e = jnp.exp2((s - jnp.max(s, axis=0, keepdims=True)) * scale)
        r = 1.0 / jnp.sum(e, axis=0, keepdims=True)
        prob[g, :, start:start + size] = (e * r).astype(jnp.bfloat16)

    half = len(order) // 2
    with jax.named_scope("relay0"):
        for i in order[:half]:
            relay(i)
    with jax.named_scope("k_relay"):
        for i, yp in enumerate(y_peers):
            j = yp * 2 + c
            remote(at(kbuf, j), at(kbuf, j), k_send.at[0], k_recv.at[yp], (j, dp)).wait_recv()
            send(at(kbuf, j), at(kbuf, j), k_fwd.at[i], k_frecv.at[yp], (sib, dp))
    with jax.named_scope("relay1"):
        for i in order[half:]:
            relay(i)
    with jax.named_scope("k_wait"):
        for yp in [y] + y_peers:
            j = yp * 2 + 1 - c
            remote(at(kbuf, j), at(kbuf, j), k_send.at[0], k_frecv.at[yp], (sib, dp)).wait_recv()
    for g in range(KVH):
        with jax.named_scope("scores"):
            weights(g, 0, GROUP * rows)

    with jax.named_scope("w_wait"):
        if n_z > 1:
            relay(back)
        for zz in [z] + z_peers:
            for xp in x_peers:
                arrived(zz * n_x + xp)
        theirs = token_part(1 - c)
        remote(theirs, theirs, t_send.at[0], t_recv.at[0], (sib, dp)).wait_recv()

    def part(head, yy, core):
        return vbuf.at[head, pl.ds(pl.multiple_of((yy * 2 + core) * rows, 16), rows), :]

    for core in range(2):
        with jax.named_scope("vproj"):
            mine = part(c, y, core)
            mine[...] = jnp.dot(
                tok[core * rows:(core + 1) * rows], wbuf[...], preferred_element_type=jnp.float32
            ).astype(jnp.bfloat16)
            for i, yp in enumerate(y_peers):
                send(mine, mine, v_send.at[core, i], v_recv.at[core, y], (yp * 2 + c, dp))
            send(mine, mine, v_send.at[core, n_y - 1], v_frecv.at[core, y], (sib, dp))
    with jax.named_scope("v_exch"):
        for core in range(2):
            for i, yp in enumerate(y_peers):
                there = part(c, yp, core)
                remote(there, there, v_send.at[0, 0], v_recv.at[core, yp], (yp * 2 + c, dp)).wait_recv()
                send(there, there, v_fwd.at[core, i], v_frecv.at[core, yp], (sib, dp))

    def attend(core):
        turned = lax.dot_general(
            vbuf[core], prob[core], (((0,), (0,)), ((), ())), preferred_element_type=jnp.float32
        )
        heads = turned.astype(jnp.bfloat16).T
        for i in range(GROUP):
            h = core * GROUP + i
            out_ref[:, pl.ds(pl.multiple_of(h * HD, HD), HD)] = heads[i * rows:(i + 1) * rows]

    with jax.named_scope("attend_c"):
        attend(c)
    with jax.named_scope("v_wait"):
        for core in range(2):
            for yp in [y] + y_peers:
                there = part(1 - c, yp, core)
                remote(there, there, v_send.at[0, 0], v_frecv.at[core, yp], (sib, dp)).wait_recv()
    with jax.named_scope("attend_o"):
        attend(1 - c)
    with jax.named_scope("wait_send"):
        for copy in pending:
            copy.wait_send()


def per_device(queries, keys, tokens, w_value, q_gain, k_gain):
    n_sp, n_dp = lax.axis_size("sp"), lax.axis_size("dp")
    n_x = inner_size(n_dp)
    n_z = n_dp // n_x
    n_y = n_sp // 2
    rows, width = tokens.shape[1:]
    depth = w_value.shape[0]
    any_spec = pl.BlockSpec(memory_space=pltpu.HBM)
    bf16, f32 = jnp.bfloat16, jnp.float32
    dma = pltpu.SemaphoreType.DMA
    length = rows * n_sp
    buffers = [
        ((rows, QH * HD), bf16),
        ((rows, KVH * HD), bf16),
        ((2 * rows, width), bf16),
        ((width, HD), bf16),
        ((length, KVH * HD), bf16),
        ((KVH, length, HD), bf16),
        ((KVH, GROUP * rows, HD), bf16),
        ((KVH, length, GROUP * rows), bf16),
        ((rows, HD), f32),
        ((rows, HD), f32),
        ((rows, HD), f32),
        ((rows, HD), f32),
        ((2 * HD, 2 * HD), bf16),
        ((1, HD), f32),
        ((1, HD), f32),
    ]
    held = sum(math.prod(shape) * jnp.dtype(kind).itemsize for shape, kind in buffers)
    limit = min(60 * 2 ** 20, held + held // 4 + 8 * rows * length * 4 + 4 * 2 ** 20)
    operands = (queries[0], keys[0], tokens[0], w_value, q_gain[None], k_gain[None])
    operands = [pltpu.with_memory_space_constraint(a, pltpu.HBM) for a in operands]
    out = pl.pallas_call(
        functools.partial(kernel, n_sp, n_dp),
        out_shape=jax.ShapeDtypeStruct((rows, QH * HD), bf16),
        in_specs=[any_spec] * 6,
        out_specs=pl.BlockSpec(memory_space=pltpu.VMEM),
        scratch_shapes=[pltpu.VMEM(shape, kind) for shape, kind in buffers]
        + [
            dma((6,)),
            dma((n_z,)),
            dma((n_z, n_x)),
            dma((n_x,)),
            dma((n_dp,)),
            dma((1,)),
            dma((1,)),
            dma((n_y,)),
            dma((n_y,)),
            dma((n_y,)),
            dma((n_y,)),
            dma((2, n_y)),
            dma((2, n_y)),
            dma((2, n_y)),
            dma((2, n_y)),
        ],
        compiler_params=pltpu.CompilerParams(
            collective_id=0, has_side_effects=True, vmem_limit_bytes=limit
        ),
        name="fused_attention",
    )(*operands)
    return out[None]


def solution(mesh):
    in_specs = (
        P("dp", "sp", None),
        P("dp", "sp", None),
        P("dp", "sp", None),
        P("dp", None),
        P(),
        P(),
    )
    return jax.shard_map(
        per_device, mesh=mesh, in_specs=in_specs, out_specs=P("dp", "sp", None), check_vma=False
    )
```

```python
import functools
import math

import jax
import jax.numpy as jnp
from jax import lax
from jax.experimental import pallas as pl
from jax.experimental.pallas import tpu as pltpu
from jax.sharding import PartitionSpec as P

HD = 128
QH = 16
KVH = 2
GRID_W = 64
GROUP = QH // KVH
epsilon = 1e-06
MESH = pl.DeviceIdType.MESH


def inner_size(n):
    size = 1
    while size * size * 4 <= n and n % (size * 2) == 0:
        size *= 2
    return size


def partner(index, d, n):
    if n & (n - 1):
        return (index + d) % n
    bit = 1
    while bit <= d:
        if d & bit:
            index = index + bit - 2 * bit * (index // bit % 2)
        bit *= 2
    return index


def kernel(
    n_sp, n_dp, q_hbm, k_hbm, tok_hbm, w_hbm, qg_hbm, kg_hbm, out_ref,
    q_in, k_in, tok, wbuf, kbuf, vbuf, qrot, prob, cos_ref, sin_ref, cosg_ref, sing_ref, perm_ref, qg_ref, kg_ref,
    v_acc, in_sem, w_z, w_x, w_d, w_recv, h_send, h_recv, t_send, t_recv, k_send, k_recv, k_fwd, k_frecv, v_send, v_recv, v_fwd, v_frecv,
):
    rows = q_hbm.shape[0]
    depth = w_hbm.shape[0]
    width = tok_hbm.shape[1]
    length = kbuf.shape[0]
    n_x = inner_size(n_dp)
    n_z = n_dp // n_x
    n_y = n_sp // 2
    sp = lax.axis_index("sp")
    dp = lax.axis_index("dp")
    z, x = dp // n_x, dp % n_x
    y, c = sp // 2, sp % 2
    sib = y * 2 + (1 - c)

    def block(d):
        return wbuf.at[pl.ds(pl.multiple_of(d * depth, 16), depth), :]

    def half(d, h):
        return wbuf.at[pl.ds(pl.multiple_of(d * depth + h * (depth // 2), 16), depth // 2), :]

    def token_part(core):
        return tok.at[pl.ds(pl.multiple_of(core * rows, 16), rows), :]

    z_peers = [partner(z, d, n_z) for d in range(1, n_z)]
    x_peers = [((x + d) % n_x) for d in range(1, n_x)]
    y_peers = [((y + d) % n_y) for d in range(1, n_y)]
    back = 0 if n_z & (n_z - 1) == 0 else n_z - 2
    diagonal = sorted({0, back}) if n_z > 1 else []
    paired = (n_x, n_y, n_z) == (2, 2, 4) and depth % 32 == 0 and width % (4 * HD) == 0
    corners = sorted(((i, j, k) for i in range(2) for j in range(2) for k in range(2) if i + j + k), key=sum)[::-1]

    def corner(i, j, k):
        return (x + i) % 2, (y + j) % 2, z + k - 2 * k * (z % 2)

    def device(xx, yy, zz):
        return (yy * 2 + c, zz * n_x + xx)

    with jax.named_scope("signal"):
        barrier = pltpu.get_barrier_semaphore()
        if paired:
            greeted = [device(x, y, partner(z, 2, n_z))] + [device(*corner(*at)) for at in corners]
        else:
            greeted = [(sp, zp * n_x + x) for zp in z_peers] + [(sp, z * n_x + xp) for xp in x_peers]
            greeted += [(sp, z_peers[i] * n_x + xp) for xp in x_peers for i in diagonal]
            greeted += [(yp * 2 + c, dp) for yp in y_peers]
        greeted.append((sib, dp))
        for where in greeted:
            pl.semaphore_signal(barrier, inc=1, device_id=where, device_id_type=MESH)

        w_mine = w_hbm.at[:, pl.ds(pl.multiple_of(c * HD, HD), HD)]
        loads = [
            pltpu.make_async_copy(src, dst, in_sem.at[i])
            for i, (src, dst) in enumerate(
                (
                    (w_mine, block(dp)), (k_hbm, k_in), (kg_hbm, kg_ref), (tok_hbm, token_part(c)),
                    (q_hbm, q_in), (qg_hbm, qg_ref),
                )
            )
        ]
        for load in loads:
            load.start()

    pending = []

    def remote(src, dst, send, recv, where):
        return pltpu.make_async_remote_copy(
            src_ref=src, dst_ref=dst, send_sem=send, recv_sem=recv, device_id=where, device_id_type=MESH
        )

    def send(*args):
        copy = remote(*args)
        copy.start()
        pending.append(copy)

    with jax.named_scope("w_send"):
        loads[0].wait()
        pl.semaphore_wait(barrier, len(greeted))
        if paired:
            mine = half(dp, y)
            send(mine, mine, h_send.at[7], h_recv.at[dp, y], device(x, y, partner(z, 2, n_z)))
            for i, at in enumerate(((1, 0, 0), (0, 0, 1), (1, 0, 1))):
                send(block(dp), block(dp), w_z.at[i], w_recv.at[dp], device(*corner(*at)))
        else:
            for k, xp in enumerate(x_peers):
                send(block(dp), block(dp), w_x.at[0, k], w_recv.at[dp], (sp, z * n_x + xp))
            for i, zp in enumerate(z_peers):
                send(block(dp), block(dp), w_z.at[i], w_recv.at[dp], (sp, zp * n_x + x))
            if n_z > 1:
                for k, xp in enumerate(x_peers):
                    send(block(dp), block(dp), w_d.at[k], w_recv.at[dp], (sp, z_peers[0] * n_x + xp))

    with jax.named_scope("tables"):
        pos = sp * rows + lax.broadcasted_iota(jnp.int32, (rows, HD), 0)
        lane = lax.broadcasted_iota(jnp.int32, (rows, HD), 1)
        grid_row = pos // GRID_W
        coord = jnp.where(lane < HD // 2, grid_row, pos - grid_row * GRID_W).astype(jnp.float32)
        step = (lax.broadcasted_iota(jnp.int32, (1, HD), 1) % (HD // 4)).astype(jnp.float32)
        angles = coord * jnp.exp2(step * (-2.0 * math.log2(10000.0) / (HD // 2)))
        cos_ref[...] = jnp.cos(angles)
        sine = jnp.sin(angles)
        sin_ref[...] = jnp.where(lane % (HD // 2) < HD // 4, -sine, sine)
        source = lax.broadcasted_iota(jnp.int32, perm_ref.shape, 0)
        target = lax.broadcasted_iota(jnp.int32, perm_ref.shape, 1)
        swapped = jnp.where(target % (HD // 2) < HD // 4, target + HD // 4, target - HD // 4)
        perm_ref[...] = (source == swapped).astype(jnp.float32).astype(jnp.bfloat16)

    def gained(gain_ref):
        gain = gain_ref[...]
        wide = jnp.broadcast_to(gain, (8, HD))
        lanes = lax.broadcasted_iota(jnp.int32, (8, HD), 1)
        other = jnp.where(
            lanes % (HD // 2) < HD // 4, pltpu.roll(wide, HD - HD // 4, 1), pltpu.roll(wide, HD // 4, 1)
        )[:1]
        cosg_ref[...] = cos_ref[...] * gain
        sing_ref[...] = sin_ref[...] * other

    def norm_rot(pair):
        other = jnp.dot(pair, perm_ref[...], preferred_element_type=jnp.float32)
        heads = []
        for j in range(2):
            u = pair[:, j * HD:(j + 1) * HD].astype(jnp.float32)
            inverse = lax.rsqrt(jnp.mean(u * u, axis=-1, keepdims=True) + epsilon)
            turned = u * cosg_ref[...] + other[:, j * HD:(j + 1) * HD] * sing_ref[...]
            heads.append((turned * inverse).astype(jnp.bfloat16))
        return heads

    def rows_of(ref, s):
        return ref.at[pl.ds(pl.multiple_of(s * rows, 16), rows), :]

    own = pl.ds(pl.multiple_of(sp * rows, 16), rows)
    with jax.named_scope("k_norm"):
        loads[1].wait()
        loads[2].wait()
        gained(kg_ref)
        for g, head in enumerate(norm_rot(k_in[...])):
            kbuf[own, g * HD:(g + 1) * HD] = head

    with jax.named_scope("k_send"):
        for i, yp in enumerate(y_peers):
            send(rows_of(kbuf, sp), rows_of(kbuf, sp), k_send.at[i], k_recv.at[y], (yp * 2 + c, dp))
        send(rows_of(kbuf, sp), rows_of(kbuf, sp), k_send.at[n_y - 1], k_frecv.at[y], (sib, dp))
        loads[3].wait()
        send(token_part(c), token_part(c), t_send.at[0], t_recv.at[0], (sib, dp))

    with jax.named_scope("q_norm"):
        loads[4].wait()
        loads[5].wait()
        gained(qg_ref)
        for b in range(QH // 2):
            for j, head in enumerate(norm_rot(q_in[:, 2 * b * HD:(2 * b + 2) * HD])):
                g, i = divmod(2 * b + j, GROUP)
                qrot[g, i * rows:(i + 1) * rows] = head

    def arrived(d):
        remote(block(d), block(d), w_z.at[0], w_recv.at[d], (sp, d)).wait_recv()

    def relay(i):
        d = z_peers[i] * n_x + x
        arrived(d)
        if i != back:
            for k, xp in enumerate(x_peers):
                send(block(d), block(d), w_x.at[i + 1, k], w_recv.at[d], (sp, z * n_x + xp))

    scale = HD ** -0.5 * math.log2(math.e)

    def weights(g, start, size):
        s = lax.dot_general(
            kbuf[:, g * HD:(g + 1) * HD], qrot[g, start:start + size], (((1,), (1,)), ((), ())),
            preferred_element_type=jnp.float32,
        )
        e = jnp.exp2((s - jnp.max(s, axis=0, keepdims=True)) * scale)
        r = 1.0 / jnp.sum(e, axis=0, keepdims=True)
        prob[g, :, start:start + size] = (e * r).astype(jnp.bfloat16)

    def half_arrived(d, h):
        remote(half(d, h), half(d, h), h_send.at[0], h_recv.at[d, h], (sp, dp)).wait_recv()

    with jax.named_scope("w_relay"):
        if paired:
            d = partner(z, 2, n_z) * n_x + x
            half_arrived(d, y)
            for i, at in enumerate(corners):
                send(half(d, y), half(d, y), h_send.at[i], h_recv.at[d, y], device(*corner(*at)))
    with jax.named_scope("k_relay"):
        for i, yp in enumerate(y_peers):
            j = yp * 2 + c
            remote(rows_of(kbuf, j), rows_of(kbuf, j), k_send.at[0], k_recv.at[yp], (j, dp)).wait_recv()
            send(rows_of(kbuf, j), rows_of(kbuf, j), k_fwd.at[i], k_frecv.at[yp], (sib, dp))
    with jax.named_scope("w_relays"):
        if not paired:
            for i in range(n_z - 1):
                if i != back:
                    relay(i)
    with jax.named_scope("k_wait"):
        for yp in [y] + y_peers:
            j = yp * 2 + 1 - c
            remote(rows_of(kbuf, j), rows_of(kbuf, j), k_send.at[0], k_frecv.at[yp], (sib, dp)).wait_recv()
    for g in range(KVH):
        with jax.named_scope("scores"):
            weights(g, 0, GROUP * rows)

    with jax.named_scope("t_wait"):
        theirs = token_part(1 - c)
        remote(theirs, theirs, t_send.at[0], t_recv.at[0], (sib, dp)).wait_recv()

    def project(core, near):
        part = (z // 2 + 1 - near) % 2 if paired else 0
        span = pl.ds(pl.multiple_of(part * (width // 2), HD), width // 2) if paired else slice(None)
        return jnp.dot(tok[core * rows:(core + 1) * rows, span], wbuf[span, :], preferred_element_type=jnp.float32)

    if paired:
        with jax.named_scope("w_near"):
            for at in ((1, 0, 0), (0, 0, 1), (1, 0, 1)):
                xx, _, zz = corner(*at)
                arrived(zz * n_x + xx)
        with jax.named_scope("vproj_near"):
            for core in range(2):
                v_acc[core * rows:(core + 1) * rows, :] = project(core, 1)
        with jax.named_scope("w_wait"):
            for at in corners:
                xx, yy, zz = corner(*at)
                half_arrived(partner(zz, 2, n_z) * n_x + xx, yy)
    else:
        with jax.named_scope("w_wait"):
            if n_z > 1:
                relay(back)
            for zz in [z] + z_peers:
                for xp in x_peers:
                    arrived(zz * n_x + xp)

    def part(head, yy, core):
        return vbuf.at[head, pl.ds(pl.multiple_of((yy * 2 + core) * rows, 16), rows), :]

    for core in range(2):
        with jax.named_scope("vproj"):
            mine = part(c, y, core)
            total = project(core, 0)
            if paired:
                total = total + v_acc[core * rows:(core + 1) * rows, :]
            mine[...] = total.astype(jnp.bfloat16)
            for i, yp in enumerate(y_peers):
                send(mine, mine, v_send.at[core, i], v_recv.at[core, y], (yp * 2 + c, dp))
            send(mine, mine, v_send.at[core, n_y - 1], v_frecv.at[core, y], (sib, dp))
    with jax.named_scope("v_exch"):
        for core in range(2):
            for i, yp in enumerate(y_peers):
                there = part(c, yp, core)
                remote(there, there, v_send.at[0, 0], v_recv.at[core, yp], (yp * 2 + c, dp)).wait_recv()
                send(there, there, v_fwd.at[core, i], v_frecv.at[core, yp], (sib, dp))

    def attend(core):
        turned = lax.dot_general(
            vbuf[core], prob[core], (((0,), (0,)), ((), ())), preferred_element_type=jnp.float32
        )
        heads = turned.astype(jnp.bfloat16).T
        for i in range(GROUP):
            h = core * GROUP + i
            out_ref[:, pl.ds(pl.multiple_of(h * HD, HD), HD)] = heads[i * rows:(i + 1) * rows]

    with jax.named_scope("attend_c"):
        attend(c)
    with jax.named_scope("v_wait"):
        for core in range(2):
            for yp in [y] + y_peers:
                there = part(1 - c, yp, core)
                remote(there, there, v_send.at[0, 0], v_frecv.at[core, yp], (sib, dp)).wait_recv()
    with jax.named_scope("attend_o"):
        attend(1 - c)
    with jax.named_scope("wait_send"):
        for copy in pending:
            copy.wait_send()


def per_device(queries, keys, tokens, w_value, q_gain, k_gain):
    n_sp, n_dp = lax.axis_size("sp"), lax.axis_size("dp")
    n_x = inner_size(n_dp)
    n_z = n_dp // n_x
    n_y = n_sp // 2
    rows, width = tokens.shape[1:]
    depth = w_value.shape[0]
    any_spec = pl.BlockSpec(memory_space=pltpu.HBM)
    bf16, f32 = jnp.bfloat16, jnp.float32
    dma = pltpu.SemaphoreType.DMA
    length = rows * n_sp
    buffers = [
        ((rows, QH * HD), bf16),
        ((rows, KVH * HD), bf16),
        ((2 * rows, width), bf16),
        ((width, HD), bf16),
        ((length, KVH * HD), bf16),
        ((KVH, length, HD), bf16),
        ((KVH, GROUP * rows, HD), bf16),
        ((KVH, length, GROUP * rows), bf16),
        ((rows, HD), f32),
        ((rows, HD), f32),
        ((rows, HD), f32),
        ((rows, HD), f32),
        ((2 * HD, 2 * HD), bf16),
        ((1, HD), f32),
        ((1, HD), f32),
        ((2 * rows, HD), f32),
    ]
    held = sum(math.prod(shape) * jnp.dtype(kind).itemsize for shape, kind in buffers)
    limit = min(60 * 2 ** 20, held + held // 4 + 8 * rows * length * 4 + 4 * 2 ** 20)
    operands = (queries[0], keys[0], tokens[0], w_value, q_gain[None], k_gain[None])
    operands = [pltpu.with_memory_space_constraint(a, pltpu.HBM) for a in operands]
    out = pl.pallas_call(
        functools.partial(kernel, n_sp, n_dp),
        out_shape=jax.ShapeDtypeStruct((rows, QH * HD), bf16),
        in_specs=[any_spec] * 6,
        out_specs=pl.BlockSpec(memory_space=pltpu.VMEM),
        scratch_shapes=[pltpu.VMEM(shape, kind) for shape, kind in buffers]
        + [
            dma((6,)),
            dma((n_z,)),
            dma((n_z, n_x)),
            dma((n_x,)),
            dma((n_dp,)),
            dma((8,)),
            dma((n_dp, 2)),
            dma((1,)),
            dma((1,)),
            dma((n_y,)),
            dma((n_y,)),
            dma((n_y,)),
            dma((n_y,)),
            dma((2, n_y)),
            dma((2, n_y)),
            dma((2, n_y)),
            dma((2, n_y)),
        ],
        compiler_params=pltpu.CompilerParams(
            collective_id=0, has_side_effects=True, vmem_limit_bytes=limit
        ),
        name="fused_attention",
    )(*operands)
    return out[None]


def solution(mesh):
    in_specs = (
        P("dp", "sp", None),
        P("dp", "sp", None),
        P("dp", "sp", None),
        P("dp", None),
        P(),
        P(),
    )
    return jax.shard_map(
        per_device, mesh=mesh, in_specs=in_specs, out_specs=P("dp", "sp", None), check_vma=False
    )
```

```python
import functools
import math

import jax
import jax.numpy as jnp
from jax import lax
from jax.experimental import pallas as pl
from jax.experimental.pallas import tpu as pltpu
from jax.sharding import PartitionSpec as P

HD = 128
QH = 16
KVH = 2
GRID_W = 64
GROUP = QH // KVH
epsilon = 1e-06
MESH = pl.DeviceIdType.MESH


def inner_size(n):
    size = 1
    while size * size * 4 <= n and n % (size * 2) == 0:
        size *= 2
    return size


def partner(index, d, n):
    if n & (n - 1):
        return (index + d) % n
    bit = 1
    while bit <= d:
        if d & bit:
            index = index + bit - 2 * bit * (index // bit % 2)
        bit *= 2
    return index


def kernel(
    n_sp, n_dp, q_hbm, k_hbm, tok_hbm, w_hbm, qg_hbm, kg_hbm, out_ref,
    q_in, k_in, tok, wbuf, kbuf, vbuf, qrot, prob, cos_ref, sin_ref, cosg_ref, sing_ref, perm_ref, qg_ref, kg_ref,
    v_acc, in_sem, w_z, w_x, w_d, w_recv, h_send, h_recv, t_send, t_recv, k_send, k_recv, k_fwd, k_frecv, v_send, v_recv, v_fwd, v_frecv,
):
    rows = q_hbm.shape[0]
    depth = w_hbm.shape[0]
    width = tok_hbm.shape[1]
    length = kbuf.shape[0]
    n_x = inner_size(n_dp)
    n_z = n_dp // n_x
    n_y = n_sp // 2
    sp = lax.axis_index("sp")
    dp = lax.axis_index("dp")
    z, x = dp // n_x, dp % n_x
    y, c = sp // 2, sp % 2
    sib = y * 2 + (1 - c)

    def block(d):
        return wbuf.at[pl.ds(pl.multiple_of(d * depth, 16), depth), :]

    def half(d, h):
        return wbuf.at[pl.ds(pl.multiple_of(d * depth + h * (depth // 2), 16), depth // 2), :]

    def token_part(core):
        return tok.at[pl.ds(pl.multiple_of(core * rows, 16), rows), :]

    z_peers = [partner(z, d, n_z) for d in range(1, n_z)]
    x_peers = [((x + d) % n_x) for d in range(1, n_x)]
    y_peers = [((y + d) % n_y) for d in range(1, n_y)]
    back = 0 if n_z & (n_z - 1) == 0 else n_z - 2
    diagonal = sorted({0, back}) if n_z > 1 else []
    paired = (n_x, n_y, n_z) == (2, 2, 4) and depth % 32 == 0 and width % (2 * HD) == 0
    corners = sorted(((i, j, k) for i in range(2) for j in range(2) for k in range(2) if i + j + k), key=sum)[::-1]

    def corner(i, j, k):
        return (x + i) % 2, (y + j) % 2, z + k - 2 * k * (z % 2)

    def device(xx, yy, zz):
        return (yy * 2 + c, zz * n_x + xx)

    with jax.named_scope("signal"):
        barrier = pltpu.get_barrier_semaphore()
        if paired:
            greeted = [device(x, y, partner(z, 2, n_z))] + [device(*corner(*at)) for at in corners]
        else:
            greeted = [(sp, zp * n_x + x) for zp in z_peers] + [(sp, z * n_x + xp) for xp in x_peers]
            greeted += [(sp, z_peers[i] * n_x + xp) for xp in x_peers for i in diagonal]
            greeted += [(yp * 2 + c, dp) for yp in y_peers]
        greeted.append((sib, dp))
        for where in greeted:
            pl.semaphore_signal(barrier, inc=1, device_id=where, device_id_type=MESH)

        w_mine = w_hbm.at[:, pl.ds(pl.multiple_of(c * HD, HD), HD)]
        loads = [
            pltpu.make_async_copy(src, dst, in_sem.at[i])
            for i, (src, dst) in enumerate(
                (
                    (w_mine, block(dp)), (k_hbm, k_in), (kg_hbm, kg_ref), (tok_hbm, token_part(c)),
                    (q_hbm, q_in), (qg_hbm, qg_ref),
                )
            )
        ]
        for load in loads:
            load.start()

    pending = []

    def remote(src, dst, send, recv, where):
        return pltpu.make_async_remote_copy(
            src_ref=src, dst_ref=dst, send_sem=send, recv_sem=recv, device_id=where, device_id_type=MESH
        )

    def send(*args):
        copy = remote(*args)
        copy.start()
        pending.append(copy)

    with jax.named_scope("w_send"):
        loads[0].wait()
        pl.semaphore_wait(barrier, len(greeted))
        if paired:
            mine = half(dp, y)
            send(mine, mine, h_send.at[7], h_recv.at[dp, y], device(x, y, partner(z, 2, n_z)))
            for i, at in enumerate(((1, 0, 0), (0, 0, 1), (1, 0, 1))):
                send(block(dp), block(dp), w_z.at[i], w_recv.at[dp], device(*corner(*at)))
        else:
            for k, xp in enumerate(x_peers):
                send(block(dp), block(dp), w_x.at[0, k], w_recv.at[dp], (sp, z * n_x + xp))
            for i, zp in enumerate(z_peers):
                send(block(dp), block(dp), w_z.at[i], w_recv.at[dp], (sp, zp * n_x + x))
            if n_z > 1:
                for k, xp in enumerate(x_peers):
                    send(block(dp), block(dp), w_d.at[k], w_recv.at[dp], (sp, z_peers[0] * n_x + xp))

    with jax.named_scope("tables"):
        pos = sp * rows + lax.broadcasted_iota(jnp.int32, (rows, HD), 0)
        lane = lax.broadcasted_iota(jnp.int32, (rows, HD), 1)
        grid_row = pos // GRID_W
        coord = jnp.where(lane < HD // 2, grid_row, pos - grid_row * GRID_W).astype(jnp.float32)
        step = (lax.broadcasted_iota(jnp.int32, (1, HD), 1) % (HD // 4)).astype(jnp.float32)
        angles = coord * jnp.exp2(step * (-2.0 * math.log2(10000.0) / (HD // 2)))
        cos_ref[...] = jnp.cos(angles)
        sine = jnp.sin(angles)
        sin_ref[...] = jnp.where(lane % (HD // 2) < HD // 4, -sine, sine)
        source = lax.broadcasted_iota(jnp.int32, perm_ref.shape, 0)
        target = lax.broadcasted_iota(jnp.int32, perm_ref.shape, 1)
        swapped = jnp.where(target % (HD // 2) < HD // 4, target + HD // 4, target - HD // 4)
        perm_ref[...] = (source == swapped).astype(jnp.float32).astype(jnp.bfloat16)

    def gained(gain_ref):
        gain = gain_ref[...]
        wide = jnp.broadcast_to(gain, (8, HD))
        lanes = lax.broadcasted_iota(jnp.int32, (8, HD), 1)
        other = jnp.where(
            lanes % (HD // 2) < HD // 4, pltpu.roll(wide, HD - HD // 4, 1), pltpu.roll(wide, HD // 4, 1)
        )[:1]
        cosg_ref[...] = cos_ref[...] * gain
        sing_ref[...] = sin_ref[...] * other

    def norm_rot(pair):
        other = jnp.dot(pair, perm_ref[...], preferred_element_type=jnp.float32)
        heads = []
        for j in range(2):
            u = pair[:, j * HD:(j + 1) * HD].astype(jnp.float32)
            inverse = lax.rsqrt(jnp.mean(u * u, axis=-1, keepdims=True) + epsilon)
            turned = u * cosg_ref[...] + other[:, j * HD:(j + 1) * HD] * sing_ref[...]
            heads.append((turned * inverse).astype(jnp.bfloat16))
        return heads

    def rows_of(ref, s):
        return ref.at[pl.ds(pl.multiple_of(s * rows, 16), rows), :]

    own = pl.ds(pl.multiple_of(sp * rows, 16), rows)
    with jax.named_scope("k_norm"):
        loads[1].wait()
        loads[2].wait()
        gained(kg_ref)
        for g, head in enumerate(norm_rot(k_in[...])):
            kbuf[own, g * HD:(g + 1) * HD] = head

    with jax.named_scope("k_send"):
        for i, yp in enumerate(y_peers):
            send(rows_of(kbuf, sp), rows_of(kbuf, sp), k_send.at[i], k_recv.at[y], (yp * 2 + c, dp))
        send(rows_of(kbuf, sp), rows_of(kbuf, sp), k_send.at[n_y - 1], k_frecv.at[y], (sib, dp))
        loads[3].wait()
        send(token_part(c), token_part(c), t_send.at[0], t_recv.at[0], (sib, dp))

    with jax.named_scope("q_norm"):
        loads[4].wait()
        loads[5].wait()
        gained(qg_ref)
        for b in range(QH // 2):
            for j, head in enumerate(norm_rot(q_in[:, 2 * b * HD:(2 * b + 2) * HD])):
                g, i = divmod(2 * b + j, GROUP)
                qrot[g, i * rows:(i + 1) * rows] = head

    def arrived(d):
        remote(block(d), block(d), w_z.at[0], w_recv.at[d], (sp, d)).wait_recv()

    def relay(i):
        d = z_peers[i] * n_x + x
        arrived(d)
        if i != back:
            for k, xp in enumerate(x_peers):
                send(block(d), block(d), w_x.at[i + 1, k], w_recv.at[d], (sp, z * n_x + xp))

    scale = HD ** -0.5 * math.log2(math.e)

    def weights(g, start, size):
        s = lax.dot_general(
            kbuf[:, g * HD:(g + 1) * HD], qrot[g, start:start + size], (((1,), (1,)), ((), ())),
            preferred_element_type=jnp.float32,
        )
        e = jnp.exp2((s - jnp.max(s, axis=0, keepdims=True)) * scale)
        r = 1.0 / jnp.sum(e, axis=0, keepdims=True)
        prob[g, :, start:start + size] = (e * r).astype(jnp.bfloat16)

    def half_arrived(d, h):
        remote(half(d, h), half(d, h), h_send.at[0], h_recv.at[d, h], (sp, dp)).wait_recv()

    with jax.named_scope("w_relay"):
        if paired:
            d = partner(z, 2, n_z) * n_x + x
            half_arrived(d, y)
            for i, at in enumerate(corners):
                send(half(d, y), half(d, y), h_send.at[i], h_recv.at[d, y], device(*corner(*at)))
    with jax.named_scope("k_relay"):
        for i, yp in enumerate(y_peers):
            j = yp * 2 + c
            remote(rows_of(kbuf, j), rows_of(kbuf, j), k_send.at[0], k_recv.at[yp], (j, dp)).wait_recv()
            send(rows_of(kbuf, j), rows_of(kbuf, j), k_fwd.at[i], k_frecv.at[yp], (sib, dp))
    with jax.named_scope("w_relays"):
        if not paired:
            for i in range(n_z - 1):
                if i != back:
                    relay(i)
    with jax.named_scope("k_wait"):
        for yp in [y] + y_peers:
            j = yp * 2 + 1 - c
            remote(rows_of(kbuf, j), rows_of(kbuf, j), k_send.at[0], k_frecv.at[yp], (sib, dp)).wait_recv()
    for g in range(KVH):
        with jax.named_scope("scores"):
            weights(g, 0, GROUP * rows)

    with jax.named_scope("t_wait"):
        theirs = token_part(1 - c)
        remote(theirs, theirs, t_send.at[0], t_recv.at[0], (sib, dp)).wait_recv()

    def project(core, near):
        part = (z // 2 + 1 - near) % 2 if paired else 0
        span = pl.ds(pl.multiple_of(part * (width // 2), HD), width // 2) if paired else slice(None)
        return jnp.dot(tok[core * rows:(core + 1) * rows, span], wbuf[span, :], preferred_element_type=jnp.float32)

    if paired:
        with jax.named_scope("w_near"):
            for at in ((1, 0, 0), (0, 0, 1), (1, 0, 1)):
                xx, _, zz = corner(*at)
                arrived(zz * n_x + xx)
        with jax.named_scope("vproj_near"):
            for core in range(2):
                v_acc[core * rows:(core + 1) * rows, :] = project(core, 1)
        with jax.named_scope("w_wait"):
            for at in corners:
                xx, yy, zz = corner(*at)
                half_arrived(partner(zz, 2, n_z) * n_x + xx, yy)
    else:
        with jax.named_scope("w_wait"):
            if n_z > 1:
                relay(back)
            for zz in [z] + z_peers:
                for xp in x_peers:
                    arrived(zz * n_x + xp)

    def part(head, yy, core):
        return vbuf.at[head, pl.ds(pl.multiple_of((yy * 2 + core) * rows, 16), rows), :]

    for core in range(2):
        with jax.named_scope("vproj"):
            mine = part(c, y, core)
            total = project(core, 0)
            if paired:
                total = total + v_acc[core * rows:(core + 1) * rows, :]
            mine[...] = total.astype(jnp.bfloat16)
            for i, yp in enumerate(y_peers):
                send(mine, mine, v_send.at[core, i], v_recv.at[core, y], (yp * 2 + c, dp))
            send(mine, mine, v_send.at[core, n_y - 1], v_frecv.at[core, y], (sib, dp))
    with jax.named_scope("v_exch"):
        for core in range(2):
            for i, yp in enumerate(y_peers):
                there = part(c, yp, core)
                remote(there, there, v_send.at[0, 0], v_recv.at[core, yp], (yp * 2 + c, dp)).wait_recv()
                send(there, there, v_fwd.at[core, i], v_frecv.at[core, yp], (sib, dp))

    def attend(core):
        turned = lax.dot_general(
            vbuf[core], prob[core], (((0,), (0,)), ((), ())), preferred_element_type=jnp.float32
        )
        heads = turned.astype(jnp.bfloat16).T
        for i in range(GROUP):
            h = core * GROUP + i
            out_ref[:, pl.ds(pl.multiple_of(h * HD, HD), HD)] = heads[i * rows:(i + 1) * rows]

    with jax.named_scope("attend_c"):
        attend(c)
    with jax.named_scope("v_wait"):
        for core in range(2):
            for yp in [y] + y_peers:
                there = part(1 - c, yp, core)
                remote(there, there, v_send.at[0, 0], v_frecv.at[core, yp], (sib, dp)).wait_recv()
    with jax.named_scope("attend_o"):
        attend(1 - c)
    with jax.named_scope("wait_send"):
        for copy in pending:
            copy.wait_send()


def per_device(queries, keys, tokens, w_value, q_gain, k_gain):
    n_sp, n_dp = lax.axis_size("sp"), lax.axis_size("dp")
    n_x = inner_size(n_dp)
    n_z = n_dp // n_x
    n_y = n_sp // 2
    rows, width = tokens.shape[1:]
    depth = w_value.shape[0]
    any_spec = pl.BlockSpec(memory_space=pltpu.HBM)
    bf16, f32 = jnp.bfloat16, jnp.float32
    dma = pltpu.SemaphoreType.DMA
    length = rows * n_sp
    buffers = [
        ((rows, QH * HD), bf16),
        ((rows, KVH * HD), bf16),
        ((2 * rows, width), bf16),
        ((width, HD), bf16),
        ((length, KVH * HD), bf16),
        ((KVH, length, HD), bf16),
        ((KVH, GROUP * rows, HD), bf16),
        ((KVH, length, GROUP * rows), bf16),
        ((rows, HD), f32),
        ((rows, HD), f32),
        ((rows, HD), f32),
        ((rows, HD), f32),
        ((2 * HD, 2 * HD), bf16),
        ((1, HD), f32),
        ((1, HD), f32),
        ((2 * rows, HD), f32),
    ]
    held = sum(math.prod(shape) * jnp.dtype(kind).itemsize for shape, kind in buffers)
    limit = min(60 * 2 ** 20, held + held // 4 + 8 * rows * length * 4 + 4 * 2 ** 20)
    operands = (queries[0], keys[0], tokens[0], w_value, q_gain[None], k_gain[None])
    operands = [pltpu.with_memory_space_constraint(a, pltpu.HBM) for a in operands]
    out = pl.pallas_call(
        functools.partial(kernel, n_sp, n_dp),
        out_shape=jax.ShapeDtypeStruct((rows, QH * HD), bf16),
        in_specs=[any_spec] * 6,
        out_specs=pl.BlockSpec(memory_space=pltpu.VMEM),
        scratch_shapes=[pltpu.VMEM(shape, kind) for shape, kind in buffers]
        + [
            dma((6,)),
            dma((n_z,)),
            dma((n_z, n_x)),
            dma((n_x,)),
            dma((n_dp,)),
            dma((8,)),
            dma((n_dp, 2)),
            dma((1,)),
            dma((1,)),
            dma((n_y,)),
            dma((n_y,)),
            dma((n_y,)),
            dma((n_y,)),
            dma((2, n_y)),
            dma((2, n_y)),
            dma((2, n_y)),
            dma((2, n_y)),
        ],
        compiler_params=pltpu.CompilerParams(
            collective_id=0, has_side_effects=True, vmem_limit_bytes=limit
        ),
        name="fused_attention",
    )(*operands)
    return out[None]


def solution(mesh):
    in_specs = (
        P("dp", "sp", None),
        P("dp", "sp", None),
        P("dp", "sp", None),
        P("dp", None),
        P(),
        P(),
    )
    return jax.shard_map(
        per_device, mesh=mesh, in_specs=in_specs, out_specs=P("dp", "sp", None), check_vma=False
    )
```
